768 devices in a mesh: ep: 48 (over z, x), tp: 16 (over y, core).
Axes of the slice: x: 4, y: 8, z: 12, core: 2. Of those that a mesh axis runs over, the one named last changes fastest.
Arguments:
- tokens: bfloat16 [1536, 4096], P('ep'), may hold values from -6 to 6
- routes: int32 [1536, 4], P('ep'), may hold values from 0 to 47, all different within a row; in each aligned block of 32 rows (0 to 31, 32 to 63, ...) at most 4 rows name the same one
- mix_weights: float32 [1536, 4], P('ep'), may hold values from 0.2 to 1
- pre_gain: float32 [4096], replicated, may hold values from 0.1 to 1.9
- gate_weight: bfloat16 [48, 4096, 2048], P('ep', None, 'tp'), may hold values from -0.09375 to 0.09375
- up_weight: bfloat16 [48, 4096, 2048], P('ep', None, 'tp'), may hold values from -0.09375 to 0.09375
- down_weight: bfloat16 [48, 2048, 4096], P('ep', 'tp'), may hold values from -1 to 1
- post_gain: float32 [4096], P('tp'), may hold values from 0.1 to 1.9
Outputs:
- layer_out: bfloat16 [1536, 4096], P('ep', 'tp')
The draws below stay inside these ranges and needn't reach their ends.
Inputs may be any that keep to these rules, and one draw needn't show every extreme that they name: `routes`: within a row the 4 experts differ; among the rows of one index of ep no expert is named more than 4 times.
All inputs are finite; a program needn't handle non-finite values.
Results may differ from the reference program's by a relative error of at most 0.019.
Values may be sent and summed in bfloat16 or wider, within the bound.
A program may use at most 32 MiB of HBM per device.

```python
import math
import jax
import jax.numpy as jnp
import numpy as np
from jax import lax

D = 4096
FF = 2048
TOP = 4
TOK_DEV = 32
EXPERTS = 48
CAP = 4
TOKENS = 1536
N_EP = 48
N_TP = 16


def draw_down_weight(key, part):
    noise = jnp.clip(jax.random.normal(jax.random.fold_in(key, 11), (EXPERTS, FF, D), jnp.float32), -6.0, 6.0)
    noise = noise * FF ** (-0.5)
    position = jnp.arange(D, dtype=jnp.float32) / D
    rise = 3.0 ** position * jax.random.uniform(jax.random.fold_in(key, 12), (D,), jnp.float32, 0.6, 1.6)
    return jnp.clip(noise * rise, -1.0, 1.0).astype(jnp.bfloat16)


def steps_of(key, shape, split, smallest, high):
    loudness = 1.0
    for axis_at, parts in split:
        steps = jax.random.uniform(jax.random.fold_in(jax.random.fold_in(key, 6), axis_at), (parts,), jnp.float32, smallest / len(split), high / len(split))
        loudness = loudness * jnp.repeat(jnp.exp(steps), shape[axis_at] // parts).reshape((-1,) + (1,) * (len(shape) - 1 - axis_at))
    return loudness


def assign_block(rng, own, number, rows, amount, top, most, skew):
    order = jax.random.permutation(rng, amount)
    packed, ordinary = portions_of(amount, rows * top, most, skew, True), portions_of(amount, rows * top, most, skew, False)
    places = jnp.arange(amount)

    def named(lengths, offset_by):
        used = int((lengths > 0).sum())
        fixed = max(1, used // 4)
        shifted = fixed + (places - fixed + offset_by * (used - fixed)) % max(1, amount - fixed)
        return jnp.zeros((amount,), jnp.int32).at[order[jnp.where(places < fixed, places, shifted)]].set(jnp.asarray(lengths, jnp.int32))

    lengths = jnp.where(number % 4 == 0, named(packed, number // 4), named(ordinary, number - number // 4 - 1))
    mixed = jax.random.permutation(jax.random.fold_in(own, 3), amount)
    giver, taker = mixed[0:amount // 2 * 2:2], mixed[1:amount // 2 * 2:2]
    margin = jnp.minimum(lengths[giver] - 1, most - lengths[taker]) // 2
    margin = jnp.where((giver == order[0]) | (taker == order[0]) | (lengths[taker] == 0), 0, jnp.maximum(margin, 0))
    shifted = jax.random.randint(jax.random.fold_in(own, 4), (amount // 2,), 0, 1 << 20) % (margin + 1)
    lengths = lengths.at[giver].add(-shifted).at[taker].add(shifted)
    labels = jnp.searchsorted(jnp.cumsum(lengths), jnp.arange(rows * top), side="right").astype(jnp.int32)
    grid = labels.reshape(top, rows).T
    grid = grid[jax.random.permutation(jax.random.fold_in(own, 1), rows)]
    offset_by = jax.random.randint(jax.random.fold_in(own, 2), (rows, 1), 0, top)
    return jnp.take_along_axis(grid, (jnp.arange(top)[None, :] + offset_by) % top, axis=1)


def portions_of(amount, total, limit, lean, full):
    portions = [(1 << 20) // math.isqrt(rank ** lean) + 1 for rank in range(1, amount + 1)]
    largest = limit if full else min(limit, max(-(-total // amount), total * portions[0] // sum(portions)))
    least = 1 if total - largest >= amount - 1 else 0
    given, surplus = [largest] + [least] * (amount - 1), total - largest - least * (amount - 1)
    while surplus > 0:
        free = [i for i in range(1, amount) if given[i] < largest] or [i for i in range(1, amount) if given[i] < limit]
        mass, left = sum([portions[i] for i in free]), surplus
        for i in free:
            extra = min(limit - given[i], max(1, left * portions[i] // mass), surplus)
            given[i] = given[i] + extra
            surplus = surplus - extra
    return np.array(given)


def bell_draw(own_key, extent, deviation, most, split=(), kind=jnp.bfloat16):
    level = steps_of(own_key, extent, split, -0.22, 0.18) if split else 1.0
    values = jax.random.normal(own_key, extent, jnp.float32) * deviation * level
    return jnp.minimum(jnp.maximum(values, -most), most).astype(kind)


def setup_inputs(seed: int = 0) -> dict:
    streams_of = jax.random.split(jax.random.key(seed), 9)
    tokens = bell_draw(streams_of[0], (TOKENS, D), 1.0, 6.0, ((0, 48),))
    routes_keys = jax.random.split(jax.random.fold_in(streams_of[1], 1), TOKENS // TOK_DEV)
    routes_turns = jax.random.permutation(jax.random.fold_in(streams_of[1], 3), TOKENS // TOK_DEV)
    routes = jax.vmap(lambda own, number: assign_block(jax.random.fold_in(streams_of[1], 2), own, number, TOK_DEV, EXPERTS, TOP, CAP, 2))(routes_keys, routes_turns).reshape((TOKENS, TOP))
    mix_weights = jnp.clip(0.2 + 0.8 * jax.random.uniform(streams_of[2], (TOKENS, TOP), jnp.float32) ** steps_of(streams_of[2], (TOKENS, TOP), ((0, 48),), -0.2, 0.2), 0.2, 1.0)
    pre_gain = jnp.clip(1.0 + 0.18 * jax.random.normal(streams_of[3], (D,), jnp.float32), 0.1, 1.9)
    gate_weight = bell_draw(streams_of[4], (EXPERTS, D, FF), D ** -0.5, 0.09375, ((0, 48), (2, 16)))
    up_weight = bell_draw(streams_of[5], (EXPERTS, D, FF), D ** -0.5, 0.09375, ((0, 48), (2, 16)))
    down_weight = draw_down_weight(jax.random.fold_in(streams_of[8], 71), 0)
    post_gain = jnp.clip(1.0 + 0.18 * jax.random.normal(streams_of[7], (D,), jnp.float32), 0.1, 1.9)
    return dict(tokens=tokens, routes=routes, mix_weights=mix_weights, pre_gain=pre_gain, gate_weight=gate_weight, up_weight=up_weight, down_weight=down_weight, post_gain=post_gain)


epsilon = 1e-06

def reference(tokens, routes, mix_weights, pre_gain, gate_weight, up_weight, down_weight, post_gain):
    floats = tokens.astype(jnp.float32)
    normed = (floats * lax.rsqrt(lax.optimization_barrier(jnp.mean(floats * floats, axis=-1, keepdims=True)) + epsilon) * pre_gain).astype(jnp.bfloat16)
    row_slots = N_EP * CAP
    group_width = FF // N_TP

    def visit_expert(result, per_expert):
        w_gate, w_up, w_down, expert_id = per_expert
        matches = routes == expert_id
        weight = lax.optimization_barrier(jnp.sum(jnp.where(matches, mix_weights, 0.0), axis=1))
        is_named = jnp.any(matches, axis=1)
        row_index = jnp.nonzero(is_named, size=row_slots, fill_value=0)[0].astype(jnp.int32)
        is_live = jnp.arange(row_slots) < jnp.sum(is_named.astype(jnp.int32))
        picked = normed[row_index]
        gate_act = jnp.dot(picked, w_gate, preferred_element_type=jnp.float32)
        up_act = jnp.dot(picked, w_up, preferred_element_type=jnp.float32)
        hidden = (jax.nn.silu(gate_act) * up_act).astype(jnp.bfloat16)
        pieces = jnp.einsum('rgf,gfd->grd', hidden.reshape(row_slots, N_TP, group_width).astype(jnp.float32), w_down.reshape(N_TP, group_width, D).astype(jnp.float32))
        pieces = lax.optimization_barrier(pieces.astype(jnp.bfloat16)).astype(jnp.float32)
        expert_out = lax.optimization_barrier(lax.optimization_barrier(jnp.sum(pieces, axis=0)).astype(jnp.bfloat16)).astype(jnp.float32)
        weighting = jnp.where(is_live, weight[row_index], 0.0)
        result = result.at[row_index].add(weighting[:, None] * expert_out)
        return (result, None)
    start = jnp.zeros((tokens.shape[0], D), jnp.float32)
    mixed, _ = lax.scan(visit_expert, start, (gate_weight, up_weight, down_weight, jnp.arange(EXPERTS, dtype=jnp.int32)))
    scale = lax.rsqrt(lax.optimization_barrier(jnp.mean(mixed * mixed, axis=-1, keepdims=True)) + epsilon)
    return (mixed * scale * post_gain).astype(jnp.bfloat16)
```

```python
import functools

import jax
import jax.numpy as jnp
from jax import lax
from jax.experimental import pallas as pl
from jax.experimental.pallas import tpu as pltpu
from jax.sharding import PartitionSpec as P

EPS = 1e-06
CAP = 4
QUARTER = 128
X_CHIPS = 4
CORES = 2
bf16, f32, i32 = jnp.bfloat16, jnp.float32, jnp.int32


def one_hot(shape, match):
    rows = lax.broadcasted_iota(i32, shape, 0)
    cols = lax.broadcasted_iota(i32, shape, 1)
    return jnp.where(match(rows, cols), 1.0, 0.0).astype(bf16)


def kernel(
    z_chips,
    x_chips,
    y_chips,
    tokens,
    routes,
    mix_weights,
    pre_gain,
    gate_weight,
    up_weight,
    down_weight,
    post_gain,
    out,
    tok,
    rts,
    mix,
    gain,
    pgain,
    wgu,
    wd,
    bt,
    mx,
    stack,
    outgoing,
    incoming,
    xf,
    acc,
    fstack,
    send_r,
    send_l,
    recv_r,
    recv_l,
    back_out,
    back_in,
    mixed,
    theirs,
    ss,
    load_sem,
    weight_sem,
    weight_send,
    weight_recv,
    out_sem,
    in_sem,
    gr_send,
    gl_send,
    gather_sem,
    sr_send,
    sl_send,
    rr_sem,
    rl_sem,
    back_send,
    back_recv,
    half_send,
    half_recv,
    ss_send,
    ss_recv,
):
    rows, width = tok.shape
    count = z_chips * x_chips // CORES
    per = count // 2
    block = width // y_chips
    quarters = block // QUARTER
    tile = quarters * CAP
    group = per * CAP
    units = wd.shape[0] // CORES
    hops = y_chips // 2
    half_x = x_chips // 2
    lanes = count * tile

    ep, tp = lax.axis_index("ep"), lax.axis_index("tp")
    z, x = ep // x_chips, ep % x_chips
    y, c = tp // CORES, tp % CORES
    partner = {"tp": y * CORES + (1 - c)}
    right = {"tp": ((y + 1) % y_chips) * CORES + c}
    left = {"tp": ((y + y_chips - 1) % y_chips) * CORES + c}

    def offset(k):
        step = k // half_x
        dz = jnp.where(step % 2 == 1, (step + 1) // 2, z_chips - step // 2) % z_chips
        return dz, c + CORES * (k % half_x)

    def ahead(k):
        dz, dx = offset(k)
        return {"ep": ((z + dz) % z_chips) * x_chips + (x + dx) % x_chips}

    def behind(k):
        dz, dx = offset(k)
        return {
            "ep": ((z + z_chips - dz) % z_chips) * x_chips + (x + x_chips - dx) % x_chips
        }

    def remote(src, dst, send, recv, device):
        return pltpu.make_async_remote_copy(
            src_ref=src,
            dst_ref=dst,
            send_sem=send,
            recv_sem=recv,
            device_id=device,
            device_id_type=pl.DeviceIdType.MESH,
        )

    barrier = pltpu.get_barrier_semaphore()

    def greet_ep(k, carry):
        @pl.when((k > 0) | (c > 0))
        def _():
            pl.semaphore_signal(
                barrier, 1, device_id=behind(k), device_id_type=pl.DeviceIdType.MESH
            )

        return carry

    def greet_tp(k, carry):
        pl.semaphore_signal(
            barrier,
            1,
            device_id={"tp": (tp + k) % (y_chips * CORES)},
            device_id_type=pl.DeviceIdType.MESH,
        )
        return carry

    lax.fori_loop(0, count, greet_ep, 0)
    lax.fori_loop(1, y_chips * CORES, greet_tp, 0)

    loads = [
        pltpu.make_async_copy(tokens, tok, load_sem.at[0]),
        pltpu.make_async_copy(routes, rts, load_sem.at[1]),
        pltpu.make_async_copy(mix_weights, mix, load_sem.at[2]),
        pltpu.make_async_copy(pre_gain, gain, load_sem.at[3]),
        pltpu.make_async_copy(post_gain, pgain, load_sem.at[4]),
    ]
    for load in loads:
        load.start()

    own_units = pl.multiple_of(c * units, units)
    gate_slot = wgu.at[:, pl.ds(own_units, units)]
    up_slot = wgu.at[:, pl.ds(pl.multiple_of((CORES + c) * units, units), units)]
    down_slot = wd.at[pl.ds(own_units, units), :]
    weights = [
        (gate_weight.at[0], gate_slot),
        (up_weight.at[0], up_slot),
        (down_weight.at[0], down_slot),
    ]
    own_weights = [
        pltpu.make_async_copy(src, dst, weight_sem.at[n]) for n, (src, dst) in enumerate(weights)
    ]
    for load in own_weights:
        load.start()
    for load in loads:
        load.wait()

    shape = (rows, lanes)
    col = lax.broadcasted_iota(i32, shape, 1)
    col_k, col_q, col_slot = col // tile, (col // CAP) % quarters, col % CAP
    dz, dx = offset(col_k)
    expert = ((z + dz) % z_chips) * x_chips + (x + dx) % x_chips
    named = jnp.zeros(shape, f32)
    weight = jnp.zeros(shape, f32)
    square = lax.broadcasted_iota(i32, (rows, rows), 0) == lax.broadcasted_iota(
        i32, (rows, rows), 1
    )
    for k in range(rts.shape[0]):
        chosen = jnp.where(square, rts[k : k + 1, :].astype(f32), 0.0)
        hit = jnp.sum(chosen, axis=1, keepdims=True) == expert.astype(f32)
        share = jnp.where(square, mix[k : k + 1, :], 0.0)
        named += jnp.where(hit, 1.0, 0.0)
        weight += jnp.where(hit, jnp.sum(share, axis=1, keepdims=True), 0.0)
    earlier = one_hot((rows, rows), lambda r, s: s < r)
    rank = jnp.dot(earlier, named.astype(bf16), preferred_element_type=f32)
    placed = jnp.where((rank == col_slot.astype(f32)) & (named > 0.0), 1.0, 0.0)
    weight = weight * placed

    floats = tok[...].astype(f32)
    scale = lax.rsqrt(jnp.mean(floats * floats, axis=-1, keepdims=True) + EPS)
    for q in range(quarters):
        part = pl.ds(q * rows, rows)
        feats = pl.ds(pl.multiple_of(y * block + q * QUARTER, QUARTER), QUARTER)
        stack[part, :] = (tok[:, feats].astype(f32) * scale * gain[:, feats]).astype(bf16)
        bt[part, :] = jnp.where(col_q == q, placed, 0.0).astype(bf16)
        w = jnp.where(col_q == q, weight, 0.0)
        high = w.astype(bf16)
        mx[part, :] = high
        mx[pl.ds((quarters + q) * rows, rows), :] = (w - high.astype(f32)).astype(bf16)
    outgoing[...] = (
        lax.dot_general(
            bt[...], stack[...], (((0,), (0,)), ((), ())), preferred_element_type=f32
        )
        .astype(bf16)
        .reshape(outgoing.shape)
    )

    waited = y_chips * CORES - 1 + count - jnp.where(c == 0, 1, 0)
    pl.semaphore_wait(barrier, waited)

    def dispatch(k, carry):
        own = (k == 0) & (c == 0)
        g = k // per

        @pl.when(own)
        def _():
            copy = pltpu.make_async_copy(outgoing.at[0], incoming.at[0], in_sem.at[0])
            copy.start()

        @pl.when(jnp.logical_not(own))
        def _():
            remote(outgoing.at[k], incoming.at[k], out_sem, in_sem.at[g], ahead(k)).start()

        return carry

    lax.fori_loop(0, count, dispatch, 0)

    sent_weights = [
        remote(src, dst, weight_send.at[n], weight_recv.at[n], partner)
        for n, (src, dst) in enumerate(weights)
    ]
    for copy in sent_weights:
        copy.start()

    size = per * tile
    sort = one_hot(
        (size, size),
        lambda r, s: (
            (s // tile == (r // CAP) % per)
            & ((s // CAP) % quarters == r // group)
            & (s % CAP == r % CAP)
        ),
    )
    unsort = one_hot(
        (size, size),
        lambda s, r: (
            (s // tile == (r // CAP) % per)
            & ((s // CAP) % quarters == r // group)
            & (s % CAP == r % CAP)
        ),
    )

    def pass_right(d, h):
        return remote(
            xf.at[(y_chips - d) % y_chips, h],
            xf.at[y_chips - d - 1, h],
            gr_send.at[d, h],
            gather_sem.at[y_chips - d - 1, h],
            right,
        )

    def pass_left(d, h):
        return remote(
            xf.at[d, h], xf.at[d + 1, h], gl_send.at[d, h], gather_sem.at[d + 1, h], left
        )

    def goes_right(d, h):
        return d < hops - 1 or (d == hops - 1 and h == 0)

    def goes_left(d, h):
        return d < hops - 1 or (d == hops - 1 and h == 1)

    for h in range(2):
        arrived = incoming.at[pl.ds(h * per, per)]
        pltpu.make_async_copy(arrived, arrived, in_sem.at[h]).wait()
        tiles = arrived[...].reshape(size, QUARTER)
        sorted_rows = jnp.dot(sort, tiles, preferred_element_type=f32).astype(bf16)
        for q in range(quarters):
            xf[0, h, :, q * QUARTER : (q + 1) * QUARTER] = sorted_rows[
                q * group : (q + 1) * group
            ]
        pass_right(0, h).start()
        pass_left(0, h).start()

    for load in own_weights:
        load.wait()
    for copy in sent_weights:
        copy.wait_recv()

    def product(o):
        depth = pl.ds(pl.multiple_of(((y + o) % y_chips) * block, block), block)
        return jnp.dot(
            xf[o].reshape(2 * group, block), wgu[depth, :], preferred_element_type=f32
        )

    acc[...] = product(0)
    for d in range(1, hops + 1):
        for h in range(2):
            if goes_right(d - 1, h):
                pass_right(d - 1, h).wait_recv()
                if goes_right(d, h):
                    pass_right(d, h).start()
            if goes_left(d - 1, h):
                pass_left(d - 1, h).wait_recv()
                if goes_left(d, h):
                    pass_left(d, h).start()
        if d < hops:
            acc[...] += product(y_chips - d) + product(d)
        else:
            acc[...] += product(d)

    gate, up = acc[:, : CORES * units], acc[:, CORES * units :]
    hidden = (gate / (1.0 + jnp.exp(-gate)) * up).astype(bf16)

    def partial(o):
        cols = pl.ds(pl.multiple_of(((y + o) % y_chips) * block, block), block)
        return jnp.dot(hidden, wd[:, cols], preferred_element_type=f32)

    def sum_right(s, h):
        return remote(
            send_r.at[s, h], recv_r.at[s - 1, h], sr_send.at[s, h], rr_sem.at[s - 1, h], right
        )

    def sum_left(s, h):
        return remote(
            send_l.at[s, h], recv_l.at[s - 1, h], sl_send.at[s, h], rl_sem.at[s - 1, h], left
        )

    last = partial(hops)
    send_r[hops, 0] = last[:group].astype(bf16)
    sum_right(hops, 0).start()
    send_l[hops, 1] = last[group:].astype(bf16)
    sum_left(hops, 1).start()
    for s in range(hops - 1, 0, -1):
        to_right, to_left = partial(s), partial(y_chips - s)
        for n in range(2):
            h = n if s < hops - 1 else 1 - n
            term = to_right[h * group : (h + 1) * group]
            if s < hops - 1 or h == 0:
                sum_right(s + 1, h).wait_recv()
                term += recv_r[s, h].astype(f32)
            send_r[s, h] = term.astype(bf16)
            sum_right(s, h).start()
            h = 1 - h
            term = to_left[h * group : (h + 1) * group]
            if s < hops - 1 or h == 1:
                sum_left(s + 1, h).wait_recv()
                term += recv_l[s, h].astype(f32)
            send_l[s, h] = term.astype(bf16)
            sum_left(s, h).start()

    own = partial(0)
    for h in range(2):
        sum_right(1, h).wait_recv()
        sum_left(1, h).wait_recv()
        total = (
            own[h * group : (h + 1) * group]
            + recv_r[0, h].astype(f32)
            + recv_l[0, h].astype(f32)
        ).astype(bf16)
        for q in range(quarters):
            fstack[h, q * group : (q + 1) * group, :] = total[:, q * QUARTER : (q + 1) * QUARTER]
        back_out[pl.ds(h * per, per)] = (
            jnp.dot(unsort, fstack[h], preferred_element_type=f32)
            .astype(bf16)
            .reshape(per, tile, QUARTER)
        )

        def give_back(k, carry, h=h):
            own = (k == 0) & (c == 0)

            @pl.when(own)
            def _():
                copy = pltpu.make_async_copy(back_out.at[k], back_in.at[k], back_recv.at[h])
                copy.start()

            @pl.when(jnp.logical_not(own))
            def _():
                remote(
                    back_out.at[k], back_in.at[k], back_send, back_recv.at[h], behind(k)
                ).start()

            return carry

        lax.fori_loop(h * per, (h + 1) * per, give_back, 0)

    total = jnp.zeros((2 * quarters * rows, QUARTER), f32)
    for h in range(2):
        arrived = back_in.at[pl.ds(h * per, per)]
        pltpu.make_async_copy(arrived, arrived, back_recv.at[h]).wait()
        total += jnp.dot(
            mx[:, h * size : (h + 1) * size],
            arrived[...].reshape(size, QUARTER),
            preferred_element_type=f32,
        )
    mixed[...] = total[: quarters * rows] + total[quarters * rows :]
    half = quarters * rows // CORES
    swap = remote(
        mixed.at[pl.ds(pl.multiple_of((1 - c) * half, half), half)],
        theirs,
        half_send,
        half_recv,
        partner,
    )
    swap.start()
    swap.wait_recv()
    final = mixed[pl.ds(pl.multiple_of(c * half, half), half), :] + theirs[...]
    final = final.reshape(quarters // CORES, rows, QUARTER)

    squares = jnp.sum(jnp.sum(final * final, axis=0), axis=-1, keepdims=True)
    diagonal = lax.broadcasted_iota(i32, (rows, QUARTER), 0) == lax.broadcasted_iota(
        i32, (rows, QUARTER), 1
    )
    ss[tp] = jnp.sum(jnp.where(diagonal, squares, 0.0), axis=0, keepdims=True)

    def tell(k, carry):
        remote(
            ss.at[tp], ss.at[tp], ss_send, ss_recv, {"tp": (tp + k) % (y_chips * CORES)}
        ).start()
        return carry

    lax.fori_loop(1, y_chips * CORES, tell, 0)
    others = ss.at[pl.ds(0, y_chips * CORES - 1)]
    pltpu.make_async_copy(others, others, ss_recv).wait()
    squares = jnp.sum(ss[...], axis=0)
    squares = jnp.sum(jnp.where(diagonal, squares, 0.0), axis=1, keepdims=True)
    scale = lax.rsqrt(squares / width + EPS)
    for q in range(quarters // CORES):
        cols = slice(q * QUARTER, (q + 1) * QUARTER)
        out[:, cols] = (final[q] * scale * pgain[:, cols]).astype(bf16)

    pltpu.make_async_copy(others, others, ss_send).wait()
    swap.wait_send()
    for copy in sent_weights:
        copy.wait_send()

    def sent(buffer, sem):
        @pl.when(c == 0)
        def _():
            most = buffer.at[pl.ds(1, count - 1)]
            pltpu.make_async_copy(most, most, sem).wait()

        @pl.when(c != 0)
        def _():
            pltpu.make_async_copy(buffer, buffer, sem).wait()

    sent(outgoing, out_sem)
    sent(back_out, back_send)
    for d in range(hops):
        for h in range(2):
            if goes_right(d, h):
                pass_right(d, h).wait_send()
                sum_right(d + 1, h).wait_send()
            if goes_left(d, h):
                pass_left(d, h).wait_send()
                sum_left(d + 1, h).wait_send()


def on_device(
    tokens, routes, mix_weights, pre_gain, gate_weight, up_weight, down_weight, post_gain
):
    rows, width = tokens.shape
    units = gate_weight.shape[2]
    experts, tps = lax.axis_size("ep"), lax.axis_size("tp")
    x_chips = min(X_CHIPS, experts // 2)
    z_chips, y_chips = experts // x_chips, tps // CORES
    count = experts // CORES
    block = width // y_chips
    quarters = block // QUARTER
    tile = quarters * CAP
    group = count // 2 * CAP
    hops = y_chips // 2
    vmem, dma = pltpu.VMEM, pltpu.SemaphoreType.DMA
    anywhere = pl.BlockSpec(memory_space=pl.ANY)
    ring = (hops + 1, 2, group, block)
    return pl.pallas_call(
        functools.partial(kernel, z_chips, x_chips, y_chips),
        out_shape=jax.ShapeDtypeStruct((rows, width // tps), bf16),
        in_specs=[anywhere] * 8,
        out_specs=pl.BlockSpec(memory_space=pltpu.VMEM),
        scratch_shapes=[
            vmem((rows, width), bf16),
            vmem(routes.shape[::-1], i32),
            vmem(mix_weights.shape[::-1], f32),
            vmem((1, width), f32),
            vmem((1, width // tps), f32),
            vmem((width, 2 * CORES * units), bf16),
            vmem((CORES * units, width), bf16),
            vmem((quarters * rows, count * tile), bf16),
            vmem((2 * quarters * rows, count * tile), bf16),
            vmem((quarters * rows, QUARTER), bf16),
            vmem((count, tile, QUARTER), bf16),
            vmem((count, tile, QUARTER), bf16),
            vmem((y_chips, 2, group, block), bf16),
            vmem((2 * group, 2 * CORES * units), f32),
            vmem((2, quarters * group, QUARTER), bf16),
            vmem(ring, bf16),
            vmem(ring, bf16),
            vmem(ring, bf16),
            vmem(ring, bf16),
            vmem((count, tile, QUARTER), bf16),
            vmem((count, tile, QUARTER), bf16),
            vmem((quarters * rows, QUARTER), f32),
            vmem((quarters * rows // CORES, QUARTER), f32),
            vmem((tps, 1, QUARTER), f32),
            dma((5,)),
            dma((3,)),
            dma((3,)),
            dma((3,)),
            dma,
            dma((2,)),
            dma((hops, 2)),
            dma((hops, 2)),
            dma((y_chips, 2)),
            dma((hops + 1, 2)),
            dma((hops + 1, 2)),
            dma((hops, 2)),
            dma((hops, 2)),
            dma,
            dma((2,)),
            dma,
            dma,
            dma,
            dma,
        ],
        compiler_params=pltpu.CompilerParams(collective_id=0, has_side_effects=True),
    )(
        tokens,
        routes.T,
        mix_weights.T,
        pre_gain.reshape(1, width),
        gate_weight,
        up_weight,
        down_weight,
        post_gain.reshape(1, width // tps),
    )


def solution(mesh):
    in_specs = (
        P("ep", None),
        P("ep", None),
        P("ep", None),
        P(),
        P("ep", None, "tp"),
        P("ep", None, "tp"),
        P("ep", "tp", None),
        P("tp"),
    )
    return jax.shard_map(
        on_device, mesh=mesh, in_specs=in_specs, out_specs=P("ep", "tp"), check_vma=False
    )
```
